256 devices in a mesh: ra: 32 (over z, y), cb: 8 (over x, core).
Axes of the slice: x: 4, y: 4, z: 8, core: 2. Of those that a mesh axis runs over, the one named last changes fastest.
Arguments:
- tokens: bfloat16 [128, 2048], P(None, 'ra'), may hold values from -6 to 6
- pre_gain: float32 [2, 2048], P(None, 'ra'), may hold values from 0.1 to 1.9
- post_gain: float32 [2, 2048], P(None, 'ra'), may hold values from 0.1 to 1.9
- gate_weight: bfloat16 [2, 2048, 5632], P(None, 'ra', 'cb'), may hold values from -0.125 to 0.125
- up_weight: bfloat16 [2, 2048, 5632], P(None, 'ra', 'cb'), may hold values from -0.125 to 0.125
- down_weight: bfloat16 [2, 5632, 2048], P(None, 'cb', 'ra'), may hold values from -0.078125 to 0.078125
Outputs:
- mixed: bfloat16 [128, 2048], P(None, 'ra')
The draws below stay inside these ranges and needn't reach their ends.
All inputs are finite; a program needn't handle non-finite values.
Results may differ from the reference program's by a relative error of at most 0.008.
Values may be sent and summed in bfloat16 or wider, within the bound.
A program may use at most 64 MiB of HBM per device.

```python
import jax
import jax.numpy as jnp
from jax import lax

D = 2048
FF = 5632
LAYERS = 2
TOKENS = 128


def with_spikes(result, key, source, target, parts, factor):
    owner, partner = [(jnp.arange(result.shape[position]) // (result.shape[position] // parts)).reshape([-1 if axis == position else 1 for axis in range(result.ndim)]) for position in (source, target)]
    chosen = jax.random.permutation(key, parts)[partner]
    strong = (owner == chosen) | (owner == (partner + parts // 2) % parts)
    return jnp.where(strong, factor * result, result)


def level_of(stream_key, extent, shards, low, high):
    gain, own = 1.0, jax.random.fold_in(stream_key, 6)
    for position, parts in shards:
        draws = jnp.exp(jax.random.uniform(jax.random.fold_in(own, position), (parts,), jnp.float32, low / len(shards), high / len(shards)))
        gain = gain * jnp.repeat(draws, extent[position] // parts).reshape([-1 if axis == position else 1 for axis in range(len(extent))])
    return gain


def bell_draw(key, extent, spread, most, shards=(), held_as=jnp.bfloat16):
    loudness = level_of(key, extent, shards, -0.22, 0.18) if shards else 1.0
    result = jax.random.normal(key, extent, jnp.float32) * spread * loudness
    return jnp.minimum(jnp.maximum(result, -most), most).astype(held_as)


def heavy_noise(stream_key, extent, deviation, reach, cuts, heavy, kind=jnp.bfloat16):
    values = deviation * jax.random.normal(stream_key, extent, jnp.float32)
    if cuts:
        values = values * level_of(stream_key, extent, cuts, -0.22, 0.18)
    return jnp.clip(with_spikes(values, jax.random.fold_in(stream_key, 3), *heavy), -reach, reach).astype(kind)


def setup_inputs(seed: int = 0) -> dict:
    key_list = jax.random.split(jax.random.key(seed), 7)
    tokens = heavy_noise(key_list[0], (TOKENS, D), 1.0, 6.0, ((1, 32),), (1, 0, 32, 2.75))
    pre_gain = jnp.clip(1.0 + 0.18 * jax.random.normal(key_list[1], (LAYERS, D), jnp.float32), 0.1, 1.9)
    post_gain = jnp.clip(1.0 + 0.18 * jax.random.normal(key_list[2], (LAYERS, D), jnp.float32), 0.1, 1.9)
    gate_weight = bell_draw(key_list[3], (LAYERS, D, FF), D ** -0.5, 0.125, ((1, 32), (2, 8)))
    up_weight = bell_draw(key_list[4], (LAYERS, D, FF), D ** -0.5, 0.125, ((1, 32), (2, 8)))
    down_weight = bell_draw(key_list[5], (LAYERS, FF, D), FF ** -0.5, 0.078125, ((1, 8), (2, 32)))
    return {"tokens": tokens, "pre_gain": pre_gain, "post_gain": post_gain, "gate_weight": gate_weight, "up_weight": up_weight, "down_weight": down_weight}


epsilon = 1e-06
residual_scale = 0.25

def reference(tokens, pre_gain, post_gain, gate_weight, up_weight, down_weight):
    stream = tokens.astype(jnp.float32)
    for sublayer in range(LAYERS):
        scale_in = lax.rsqrt(lax.optimization_barrier(jnp.mean(stream * stream, axis=1, keepdims=True)) + epsilon)
        normed = (stream * scale_in * pre_gain[sublayer]).astype(jnp.bfloat16)
        gate_sum = jnp.dot(normed, gate_weight[sublayer], preferred_element_type=jnp.float32)
        up_sum = jnp.dot(normed, up_weight[sublayer], preferred_element_type=jnp.float32)
        hidden = (jax.nn.silu(gate_sum) * up_sum).astype(jnp.bfloat16)
        branch = jnp.dot(hidden, down_weight[sublayer], preferred_element_type=jnp.float32)
        scale_out = lax.rsqrt(lax.optimization_barrier(jnp.mean(branch * branch, axis=1, keepdims=True)) + epsilon)
        stream = residual_scale * stream + branch * scale_out * post_gain[sublayer]
    return stream.astype(jnp.bfloat16)
```

```python
import functools

import jax
import jax.numpy as jnp
from jax import lax
from jax.experimental import pallas as pl
from jax.experimental.pallas import tpu as pltpu
from jax.sharding import PartitionSpec as P

MESH = pl.DeviceIdType.MESH
F32, BF16 = jnp.float32, jnp.bfloat16

D = 2048
EPSILON = 1e-06
RESIDUAL = 0.25
NY, NZ, NC = 4, 8, 8
NR = NY * NZ
TOKENS = 128
ROWS = TOKENS // NZ
FEATURES = D // NR
UNITS = 704
MAIN, REST = 128, 48
STAT = 96


def terms(value):
    high = value.astype(BF16).astype(F32)
    left = value - high
    middle = left.astype(BF16).astype(F32)
    return [high, middle, left - middle]


def joined(tile, lane):
    return tile[:, lane : lane + 1] + tile[:, lane + 1 : lane + 2] + tile[:, lane + 2 : lane + 3]


def silu(value):
    return value / (1.0 + jnp.exp(-value))


def kernel(
    tokens_hbm, pre_hbm, post_hbm, gate_hbm, up_hbm, down_hbm, out_ref,
    tokens_v, gains_v, gate_v, up_v, down_v, wide_v, tall_v,
    sent_v, got_v, mine_v, hidden_v, part_v, parts_v, norm_v, norms_v,
    load_sem, send_sem, recv_sem,
):
    r, c = lax.axis_index("ra"), lax.axis_index("cb")
    z, y = r // NY, r % NY

    def plane(k):
        other = k + 1
        dz, dy = other // NY, other % NY
        there_z, there_y = lax.rem(z + dz, NZ), lax.rem(y + dy, NY)
        return other, there_z, there_y, there_z * NY + there_y

    barrier = pltpu.get_barrier_semaphore()

    def greet_plane(k, carry):
        pl.semaphore_signal(barrier, inc=1, device_id={"ra": plane(k)[3]}, device_id_type=MESH)
        return carry

    def greet_row(k, carry):
        pl.semaphore_signal(barrier, inc=1, device_id={"cb": lax.rem(c + k + 1, NC)}, device_id_type=MESH)
        return carry

    lax.fori_loop(0, NR - 1, greet_plane, 0)
    lax.fori_loop(0, NC - 1, greet_row, 0)

    loads = [
        pltpu.make_async_copy(tokens_hbm, tokens_v, load_sem.at[0]),
        pltpu.make_async_copy(pre_hbm, gains_v.at[0], load_sem.at[1]),
        pltpu.make_async_copy(post_hbm, gains_v.at[1], load_sem.at[2]),
        pltpu.make_async_copy(gate_hbm, gate_v, load_sem.at[3]),
        pltpu.make_async_copy(up_hbm, up_v, load_sem.at[4]),
        pltpu.make_async_copy(down_hbm, down_v, load_sem.at[5]),
    ]
    for load in loads:
        load.start()
    for load in loads:
        load.wait()

    def square(value):
        rows, lanes = value.shape
        if rows < 128:
            value = jnp.concatenate([value, jnp.zeros((128 - rows, lanes), F32)], axis=0)
        if lanes < 128:
            value = jnp.concatenate([value, jnp.zeros((value.shape[0], 128 - lanes), F32)], axis=1)
        return value.T

    row = lax.broadcasted_iota(jnp.int32, (64, 128), 0)
    lane = lax.broadcasted_iota(jnp.int32, (64, 128), 1)
    passing = jnp.where(row == lane - STAT, 1.0, 0.0).astype(BF16)
    nothing = jnp.zeros((64, 128), BF16)
    for l in range(2):
        gate_tail = gate_v[l, :, 512:704].astype(F32)
        up_tail = up_v[l, :, 512:704].astype(F32)
        pad = jnp.zeros((64, 64), F32)
        gate_tail = jnp.concatenate([gate_tail, pad], axis=1)
        up_tail = jnp.concatenate([up_tail, pad], axis=1)
        for q in range(NY):
            wide_v[l, 0:64, q * 384 : q * 384 + 128] = gate_v[l, :, q * 128 : q * 128 + 128]
            wide_v[l, 0:64, q * 384 + 128 : q * 384 + 256] = up_v[l, :, q * 128 : q * 128 + 128]
            gate_rest = pltpu.roll(gate_tail, (256 - REST * q) % 256, 1)[:, 0:128] if q else gate_tail[:, 0:128]
            up_rest = pltpu.roll(up_tail, (256 + REST - REST * q) % 256, 1)[:, 0:128] if q != 1 else up_tail[:, 0:128]
            rest = jnp.where(lane < REST, gate_rest, jnp.where(lane < 2 * REST, up_rest, 0.0))
            wide_v[l, 0:64, q * 384 + 256 : q * 384 + 384] = rest.astype(BF16)
            wide_v[l, 64:128, q * 384 : q * 384 + 128] = nothing
            wide_v[l, 64:128, q * 384 + 128 : q * 384 + 256] = nothing
            wide_v[l, 64:128, q * 384 + 256 : q * 384 + 384] = passing

    pick_row = lax.broadcasted_iota(jnp.int32, (16, 128), 0)
    pick_lane = lax.broadcasted_iota(jnp.int32, (16, 128), 1)
    pick = jnp.where((pick_row == 0) & (pick_lane >= REST) & (pick_lane < REST + 3), 1.0, 0.0).astype(BF16)
    for l in range(2):
        for q in range(NY):
            main = down_v[l, q * MAIN : q * MAIN + MAIN, :].astype(F32)
            rest = down_v[l, 512 + q * REST : 512 + q * REST + REST, :].astype(F32)
            tall_v[l, 0:64, q * 256 : q * 256 + 128] = square(main)[0:64].astype(BF16)
            tall_v[l, 0:64, q * 256 + 128 : q * 256 + 256] = square(rest)[0:64].astype(BF16)
            tall_v[l, 64:80, q * 256 : q * 256 + 128] = jnp.zeros((16, 128), BF16)
            tall_v[l, 64:80, q * 256 + 128 : q * 256 + 256] = pick if q == 0 else jnp.zeros((16, 128), BF16)

    stream0 = square(tokens_v[...].astype(F32))[0:64]
    gains = [square(jnp.concatenate([gains_v[i], jnp.zeros((6, 64), F32)], axis=0))[0:64] for i in range(2)]
    pre = [gains[0][:, l : l + 1] for l in range(2)]
    post = [gains[1][:, l : l + 1] for l in range(2)]

    def multiply(l, slot, features, statistics):
        lines = [t for s in statistics for t in terms(s)]
        lines = jnp.concatenate(lines + [jnp.zeros((64 - len(lines), 128), F32)], axis=0) if lines else jnp.zeros((64, 128), F32)
        left = jnp.concatenate([features, lines], axis=0).T
        high = left.astype(BF16)
        low = (left - high.astype(F32)).astype(BF16)
        for q in range(NY):
            wide = wide_v[l, :, q * 384 : q * 384 + 384]
            part = jnp.dot(high, wide, preferred_element_type=F32) + jnp.dot(low, wide, preferred_element_type=F32)
            sent_v[slot, :, q] = part.reshape(NZ, ROWS, 384).astype(BF16)

    def scatter(slot):
        def step(k, carry):
            other, tz, ty, there = plane(k)
            pltpu.make_async_remote_copy(
                src_ref=sent_v.at[slot, tz, ty],
                dst_ref=got_v.at[slot, other],
                send_sem=send_sem.at[slot],
                recv_sem=recv_sem.at[slot],
                device_id={"ra": there},
                device_id_type=MESH,
            ).start()
            return carry

        lax.fori_loop(0, NR - 1, step, 0)

    def all_of(ref, sem):
        pltpu.make_async_copy(ref, ref, sem).wait()

    def total(slot):
        all_of(got_v.at[slot, pl.ds(1, NR - 1)], recv_sem.at[slot])
        acc = sent_v[slot, z, y].astype(F32)
        for k in range(1, NR):
            acc = acc + got_v[slot, k].astype(F32)
        return acc

    small_lane = lax.broadcasted_iota(jnp.int32, (ROWS, 128), 1)

    def activate(main_gate, main_up, rest_tile, extra):
        main = silu(main_gate) * main_up
        rest = silu(rest_tile) * pltpu.roll(rest_tile, 128 - REST, 1)
        rest = jnp.where(small_lane < REST, rest, 0.0)
        if extra is not None:
            for i, term in enumerate(terms(extra)):
                rest = jnp.where(small_lane == REST + i, term, rest)
        return main.astype(BF16), rest.astype(BF16)

    def broadcast_hidden(l, pair):
        mine_v[l, :, 0:128] = pair[0]
        mine_v[l, :, 128:256] = pair[1]

        def step(k, carry):
            pltpu.make_async_remote_copy(
                src_ref=mine_v.at[l],
                dst_ref=hidden_v.at[l, y, z],
                send_sem=send_sem.at[3 + l],
                recv_sem=recv_sem.at[3 + l],
                device_id={"ra": plane(k)[3]},
                device_id_type=MESH,
            ).start()
            return carry

        lax.fori_loop(0, NR - 1, step, 0)
        hidden_v[l, y, z, :, 0:128] = pair[0]
        hidden_v[l, y, z, :, 128:256] = pair[1]

    def project(l):
        all_of(got_v.at[0, pl.ds(1, NR - 1), :, pl.ds(0, 256)], recv_sem.at[3 + l])
        acc = jnp.zeros((80, 128), F32)
        for q in range(NY):
            right = hidden_v[l, q].reshape(TOKENS, 256)
            acc = acc + lax.dot_general(
                tall_v[l, :, q * 256 : q * 256 + 256], right, (((1,), (1,)), ((), ())), preferred_element_type=F32
            )
        return acc

    def branch_total(l, part):
        part_v[l] = part.astype(BF16)

        def step(k, carry):
            pltpu.make_async_remote_copy(
                src_ref=part_v.at[l],
                dst_ref=parts_v.at[l, c],
                send_sem=send_sem.at[5 + l],
                recv_sem=recv_sem.at[5 + l],
                device_id={"cb": lax.rem(c + k + 1, NC)},
                device_id_type=MESH,
            ).start()
            return carry

        lax.fori_loop(0, NC - 1, step, 0)
        parts_v[l, c] = part.astype(BF16)
        all_of(parts_v.at[l, pl.ds(0, NC - 1)], recv_sem.at[5 + l])
        acc = parts_v[l, 0].astype(F32)
        for k in range(1, NC):
            acc = acc + parts_v[l, k].astype(F32)
        return acc

    def over_features(value):
        return jnp.sum(value, axis=0, keepdims=True)

    multiply(0, 0, stream0 * pre[0], [over_features(stream0 * stream0)])
    pl.semaphore_wait(barrier, NR - 1 + NC - 1)
    scatter(0)
    multiply(1, 1, stream0 * pre[1], [])
    acc = total(0)
    squares = joined(acc[:, 256:384], STAT)
    scale = lax.rsqrt(squares / D + EPSILON)
    acc = acc * scale
    broadcast_hidden(0, activate(acc[:, 0:128], acc[:, 128:256], acc[:, 256:384], None))
    scatter(1)
    branch = branch_total(0, project(0)[0:64])
    gained = branch * post[0]

    multiply(1, 2, gained * pre[1], [over_features(branch * branch), over_features(gained * gained), over_features(stream0 * gained)])
    scatter(2)
    early = total(1)
    acc = total(2)
    rest = acc[:, 256:384]
    scale_out = lax.rsqrt(joined(rest, STAT) / D + EPSILON)
    squares = (
        RESIDUAL * RESIDUAL * squares
        + 2.0 * RESIDUAL * scale_out * joined(rest, STAT + 6)
        + scale_out * scale_out * joined(rest, STAT + 3)
    )
    scale = lax.rsqrt(squares / D + EPSILON)
    acc = scale * (RESIDUAL * early + scale_out * acc)
    broadcast_hidden(1, activate(acc[:, 0:128], acc[:, 128:256], acc[:, 256:384], scale_out))
    both = project(1)
    stream1 = RESIDUAL * stream0 + gained * both[64:65]
    branch = branch_total(1, both[0:64])
    norm_v[...] = over_features(branch * branch)

    def tell(k, carry):
        pltpu.make_async_remote_copy(
            src_ref=norm_v,
            dst_ref=norms_v.at[r],
            send_sem=send_sem.at[7],
            recv_sem=recv_sem.at[7],
            device_id={"ra": plane(k)[3]},
            device_id_type=MESH,
        ).start()
        return carry

    lax.fori_loop(0, NR - 1, tell, 0)
    norms_v[r] = norm_v[...]
    all_of(norms_v.at[pl.ds(0, NR - 1)], recv_sem.at[7])
    norm = norms_v[0]
    for k in range(1, NR):
        norm = norm + norms_v[k]
    scale_out = lax.rsqrt(norm / D + EPSILON)
    stream2 = RESIDUAL * stream1 + branch * post[1] * scale_out
    out_ref[...] = square(stream2)[:, 0:64].astype(BF16)

    for slot in range(3):
        all_of(got_v.at[slot, pl.ds(1, NR - 1)], send_sem.at[slot])
    for l in range(2):
        all_of(got_v.at[0, pl.ds(1, NR - 1), :, pl.ds(0, 256)], send_sem.at[3 + l])
        all_of(parts_v.at[l, pl.ds(0, NC - 1)], send_sem.at[5 + l])
    all_of(norms_v.at[pl.ds(0, NR - 1)], send_sem.at[7])


def per_device(tokens, pre_gain, post_gain, gate_weight, up_weight, down_weight):
    return pl.pallas_call(
        kernel,
        out_shape=jax.ShapeDtypeStruct((TOKENS, FEATURES), BF16),
        in_specs=[pl.BlockSpec(memory_space=pl.ANY)] * 6,
        out_specs=pl.BlockSpec(memory_space=pltpu.VMEM),
        scratch_shapes=[
            pltpu.VMEM((TOKENS, FEATURES), BF16),
            pltpu.VMEM((2, 2, FEATURES), F32),
            pltpu.VMEM((2, FEATURES, UNITS), BF16),
            pltpu.VMEM((2, FEATURES, UNITS), BF16),
            pltpu.VMEM((2, UNITS, FEATURES), BF16),
            pltpu.VMEM((2, 128, NY * 384), BF16),
            pltpu.VMEM((2, 80, NY * 256), BF16),
            pltpu.VMEM((3, NZ, NY, ROWS, 384), BF16),
            pltpu.VMEM((3, NR, ROWS, 384), BF16),
            pltpu.VMEM((2, ROWS, 256), BF16),
            pltpu.VMEM((2, NY, NZ, ROWS, 256), BF16),
            pltpu.VMEM((2, FEATURES, TOKENS), BF16),
            pltpu.VMEM((2, NC, FEATURES, TOKENS), BF16),
            pltpu.VMEM((1, TOKENS), F32),
            pltpu.VMEM((NR, 1, TOKENS), F32),
            pltpu.SemaphoreType.DMA((6,)),
            pltpu.SemaphoreType.DMA((8,)),
            pltpu.SemaphoreType.DMA((8,)),
        ],
        compiler_params=pltpu.CompilerParams(collective_id=0, has_side_effects=True),
    )(tokens, pre_gain, post_gain, gate_weight, up_weight, down_weight)


def solution(mesh):
    return jax.shard_map(
        per_device,
        mesh=mesh,
        in_specs=(
            P(None, "ra"),
            P(None, "ra"),
            P(None, "ra"),
            P(None, "ra", "cb"),
            P(None, "ra", "cb"),
            P(None, "cb", "ra"),
        ),
        out_specs=P(None, "ra"),
        check_vma=False,
    )
```

```python
import jax
import jax.numpy as jnp
from jax import lax
from jax.experimental import pallas as pl
from jax.experimental.pallas import tpu as pltpu
from jax.sharding import PartitionSpec as P

MESH = pl.DeviceIdType.MESH
F32, BF16 = jnp.float32, jnp.bfloat16

D = 2048
EPSILON = 1e-06
RESIDUAL = 0.25
NY, NZ, NC = 4, 8, 8
NR = NY * NZ
TOKENS = 128
ROWS = TOKENS // NZ
FEATURES = D // NR
UNITS = 704
REST = 48
STAT = 96
Z_ORDER = (4, 3, 5, 2, 6, 1, 7)
Y_ORDER = (2, 1, 3)


def terms(value):
    high = value.astype(BF16).astype(F32)
    left = value - high
    middle = left.astype(BF16).astype(F32)
    return [high, middle, left - middle]


def joined(tile, lane):
    return tile[:, lane : lane + 1] + tile[:, lane + 1 : lane + 2] + tile[:, lane + 2 : lane + 3]


def silu(value):
    return value / (1.0 + jnp.exp(-value))


def over_features(value):
    return jnp.sum(value, axis=0, keepdims=True)


def all_of(ref, sem):
    pltpu.make_async_copy(ref, ref, sem).wait()


def kernel(
    tokens_hbm, pre_hbm, post_hbm, gate_hbm, up_hbm, down_hbm, out_ref,
    tokens_v, gains_v, gate_v, up_v, down_v, tokens4_v, gains4_v,
    wide_from_v, wide_v, tall_from_v, tall_v,
    square_v, squares_v, sent_v, got_v, mine_v, hidden_v,
    piece_v, own_v, pieces_v, part_v, parts_v, block_v, branch_v, stream_v, gained_v, norm_v, norms_v,
    load_sem, send_sem, recv_sem,
):
    r, c = lax.axis_index("ra"), lax.axis_index("cb")
    z, y = r // NY, r % NY
    pending = []

    def to_z(dz):
        there = lax.rem(z + dz, NZ)
        return there, {"ra": there * NY + y}

    def to_y(dy):
        there = lax.rem(y + dy, NY)
        return there, {"ra": z * NY + there}

    def to_c(dc):
        there = lax.rem(c + dc, NC)
        return there, {"cb": there}

    def push(src, dst, which, device):
        pltpu.make_async_remote_copy(
            src_ref=src, dst_ref=dst, send_sem=send_sem.at[which], recv_sem=recv_sem.at[which],
            device_id=device, device_id_type=MESH,
        ).start()

    barrier = pltpu.get_barrier_semaphore()
    for device in [to_z(k)[1] for k in range(1, NZ)] + [to_y(k)[1] for k in range(1, NY)] + [to_c(k)[1] for k in range(1, NC)]:
        pl.semaphore_signal(barrier, inc=1, device_id=device, device_id_type=MESH)

    loads = [
        pltpu.make_async_copy(gate_hbm, gate_v, load_sem.at[0]),
        pltpu.make_async_copy(up_hbm, up_v, load_sem.at[1]),
        pltpu.make_async_copy(tokens_hbm, tokens_v, load_sem.at[2]),
        pltpu.make_async_copy(pre_hbm, gains_v.at[0], load_sem.at[3]),
        pltpu.make_async_copy(post_hbm, gains_v.at[1], load_sem.at[4]),
        pltpu.make_async_copy(down_hbm, down_v, load_sem.at[5]),
    ]
    for load in loads:
        load.start()

    lane64 = lax.broadcasted_iota(jnp.int32, (FEATURES, 128), 1)

    def tail(ref, l):
        return jnp.concatenate([ref[l, :, 512:704].astype(F32), jnp.zeros((FEATURES, 64), F32)], axis=1)

    def shifted(value, lanes):
        lanes = lanes % 256
        return pltpu.roll(value, lanes, 1)[:, 0:128] if lanes else value[:, 0:128]

    def arrange_wide(l):
        gate_tail, up_tail = tail(gate_v, l), tail(up_v, l)
        for q in range(NY):
            wide_from_v[l, q, :, 0:128] = gate_v[l, :, q * 128 : q * 128 + 128]
            wide_from_v[l, q, :, 128:256] = up_v[l, :, q * 128 : q * 128 + 128]
            rest = jnp.where(
                lane64 < REST, shifted(gate_tail, -REST * q), jnp.where(lane64 < 2 * REST, shifted(up_tail, REST - REST * q), 0.0)
            )
            wide_from_v[l, q, :, 256:384] = rest.astype(BF16)

    def arrange_tall(l):
        down_tail = tail(down_v, l)
        for q in range(NY):
            tall_from_v[l, q, :, 0:128] = down_v[l, :, q * 128 : q * 128 + 128]
            tall_from_v[l, q, :, 128:256] = jnp.where(lane64 < REST, shifted(down_tail, -REST * q), 0.0).astype(BF16)

    def exchange_wide(l):
        for dy in Y_ORDER:
            there, device = to_y(dy)
            push(wide_from_v.at[l, there], wide_v.at[l, y], l, device)
        wide_v[l, y] = wide_from_v[l, y]
        pending.append((wide_from_v.at[l, pl.ds(0, NY - 1)], send_sem.at[l]))

    def exchange_tall(l):
        for dy in Y_ORDER:
            there, device = to_y(dy)
            push(tall_from_v.at[l, there], tall_v.at[l, y], 2 + l, device)
        tall_v[l, y] = tall_from_v[l, y]
        pending.append((tall_from_v.at[l, pl.ds(0, NY - 1)], send_sem.at[2 + l]))

    loads[0].wait()
    loads[1].wait()
    arrange_wide(0)
    for load in loads[2:]:
        load.wait()
    pl.semaphore_wait(barrier, NZ - 1 + NY - 1 + NC - 1)


    for dy in Y_ORDER:
        push(tokens_v, tokens4_v.at[y], 4, to_y(dy)[1])
        push(gains_v, gains4_v.at[y], 5, to_y(dy)[1])
    tokens4_v[y] = tokens_v[...]
    gains4_v[y] = gains_v[...]
    pending.append((tokens4_v.at[pl.ds(0, NY - 1)], send_sem.at[4]))
    pending.append((gains4_v.at[pl.ds(0, NY - 1)], send_sem.at[5]))
    exchange_wide(0)

    arrange_tall(0)
    exchange_tall(0)
    all_of(tokens4_v.at[pl.ds(0, NY - 1)], recv_sem.at[4])
    stream0 = tokens4_v[...].reshape(NY * FEATURES, TOKENS).astype(F32)
    own_square = over_features(stream0 * stream0)
    square_v[...] = own_square
    for dz in Z_ORDER:
        push(square_v, squares_v.at[z], 6, to_z(dz)[1])
    squares_v[z] = own_square
    pending.append((squares_v.at[pl.ds(0, NZ - 1)], send_sem.at[6]))
    arrange_wide(1)
    exchange_wide(1)
    arrange_tall(1)
    exchange_tall(1)

    all_of(gains4_v.at[pl.ds(0, NY - 1)], recv_sem.at[5])
    lines = []
    for q in range(NY):
        lines += [gains4_v[q, 0], gains4_v[q, 1], jnp.zeros((4, FEATURES), F32)]
    lines = jnp.concatenate(lines + [jnp.zeros((128 - 8 * NY, FEATURES), F32)], axis=0)
    columns = jnp.concatenate([lines, jnp.zeros((128, 128 - FEATURES), F32)], axis=1).T[0:FEATURES]

    def gain(i):
        return jnp.concatenate([columns[:, 8 * q + i : 8 * q + i + 1] for q in range(NY)], axis=0)


    passing = jnp.where(
        lax.broadcasted_iota(jnp.int32, (128, 128), 0) == lax.broadcasted_iota(jnp.int32, (128, 128), 1) - STAT, 1.0, 0.0
    ).astype(BF16)

    def multiply(l, slot, features, statistics, exact):
        left = features.T
        high = left.astype(BF16)
        wide = wide_v[l].reshape(NY * FEATURES, 384)
        part = jnp.dot(high, wide, preferred_element_type=F32)
        if not exact:
            low = (left - high.astype(F32)).astype(BF16)
            part = part + jnp.dot(low, wide, preferred_element_type=F32)
        last = part[:, 256:384]
        if statistics:
            lines = [t for s in statistics for t in terms(s)]
            lines = jnp.concatenate(lines + [jnp.zeros((128 - len(lines), 128), F32)], axis=0)
            last = last + jnp.dot(lines.T.astype(BF16), passing, preferred_element_type=F32)
        sent_v[slot, :, :, 0:256] = part[:, 0:256].reshape(NZ, ROWS, 256).astype(BF16)
        sent_v[slot, :, :, 256:384] = last.reshape(NZ, ROWS, 128).astype(BF16)

    def scatter(slot):
        for dz in Z_ORDER:
            there, device = to_z(dz)
            push(sent_v.at[slot, there], got_v.at[slot, dz], 7 + slot, device)
        pending.append((got_v.at[slot, pl.ds(1, NZ - 1)], send_sem.at[7 + slot]))

    def total(slot):
        all_of(got_v.at[slot, pl.ds(1, NZ - 1)], recv_sem.at[7 + slot])
        acc = sent_v[slot, z].astype(F32)
        for k in range(1, NZ):
            acc = acc + got_v[slot, k].astype(F32)
        return acc

    small_lane = lax.broadcasted_iota(jnp.int32, (ROWS, 128), 1)

    def broadcast_hidden(l, acc, extra):
        rest = acc[:, 256:384]
        main = silu(acc[:, 0:128]) * acc[:, 128:256]
        rest = jnp.where(small_lane < REST, silu(rest) * pltpu.roll(rest, 128 - REST, 1), 0.0)
        if extra is not None:
            for i, term in enumerate(terms(extra)):
                rest = jnp.where(small_lane == REST + i, term, rest)
        both = jnp.concatenate([main, rest], axis=1).astype(BF16)
        mine_v[l] = both
        for dz in Z_ORDER:
            push(mine_v.at[l], hidden_v.at[l, z], 10 + l, to_z(dz)[1])
        hidden_v[l, z] = both
        pending.append((hidden_v.at[l, pl.ds(0, NZ - 1)], send_sem.at[10 + l]))

    def project(l):
        all_of(tall_v.at[l, pl.ds(0, NY - 1)], recv_sem.at[2 + l])
        all_of(hidden_v.at[l, pl.ds(0, NZ - 1)], recv_sem.at[10 + l])
        right = hidden_v[l].reshape(TOKENS, 256)
        return lax.dot_general(
            tall_v[l].reshape(NY * FEATURES, 256), right, (((1,), (1,)), ((), ())), preferred_element_type=F32
        )

    def branch_total(l, part):
        part = part.reshape(NY, FEATURES, TOKENS)
        piece_v[l] = part.astype(BF16)
        for dy in Y_ORDER:
            there, device = to_y(dy)
            push(piece_v.at[l, there], pieces_v.at[l, dy], 12 + l, device)
        own_v[...] = part
        pending.append((pieces_v.at[l, pl.ds(1, NY - 1)], send_sem.at[12 + l]))
        all_of(pieces_v.at[l, pl.ds(1, NY - 1)], recv_sem.at[12 + l])
        acc = own_v[y]
        for k in range(1, NY):
            acc = acc + pieces_v[l, k].astype(F32)
        rounded = acc.astype(BF16)
        part_v[l] = rounded
        for dc in range(1, NC):
            push(part_v.at[l], parts_v.at[l, c], 14 + l, to_c(dc)[1])
        parts_v[l, c] = rounded
        pending.append((parts_v.at[l, pl.ds(0, NC - 1)], send_sem.at[14 + l]))
        all_of(parts_v.at[l, pl.ds(0, NC - 1)], recv_sem.at[14 + l])
        acc = parts_v[l, 0].astype(F32)
        for k in range(1, NC):
            acc = acc + parts_v[l, k].astype(F32)
        return acc

    gains = [gain(i) for i in range(3)]
    all_of(squares_v.at[pl.ds(0, NZ - 1)], recv_sem.at[6])
    squares = squares_v[0]
    for k in range(1, NZ):
        squares = squares + squares_v[k]
    scale = lax.rsqrt(squares / D + EPSILON)
    all_of(wide_v.at[0, pl.ds(0, NY - 1)], recv_sem.at[0])
    multiply(0, 0, stream0 * scale * gains[0], [], True)
    scatter(0)
    all_of(wide_v.at[1, pl.ds(0, NY - 1)], recv_sem.at[1])
    multiply(1, 1, stream0 * gains[1], [own_square], False)
    acc = total(0)
    broadcast_hidden(0, acc, None)
    scatter(1)
    part = project(0)
    block = branch_total(0, part)
    block_v[...] = block
    for dy in Y_ORDER:
        push(block_v, branch_v.at[y], 16, to_y(dy)[1])
    branch_v[y] = block
    pending.append((branch_v.at[pl.ds(0, NY - 1)], send_sem.at[16]))
    all_of(branch_v.at[pl.ds(0, NY - 1)], recv_sem.at[16])
    branch = branch_v[...].reshape(NY * FEATURES, TOKENS)
    gained = branch * gains[2]

    multiply(1, 2, gained * gains[1], [over_features(branch * branch), over_features(gained * gained), over_features(stream0 * gained)], False)
    scatter(2)
    stream_v[...] = stream0.reshape(NY, FEATURES, TOKENS)
    gained_v[...] = gained.reshape(NY, FEATURES, TOKENS)
    early = total(1)
    acc = total(2)
    rest = acc[:, 256:384]
    scale_out = lax.rsqrt(joined(rest, STAT) / D + EPSILON)
    squares = (
        RESIDUAL * RESIDUAL * joined(early[:, 256:384], STAT)
        + 2.0 * RESIDUAL * scale_out * joined(rest, STAT + 6)
        + scale_out * scale_out * joined(rest, STAT + 3)
    )
    scale = lax.rsqrt(squares / D + EPSILON)
    acc = scale * (RESIDUAL * early + scale_out * acc)
    broadcast_hidden(1, acc, scale_out)
    part = project(1)
    picked = jnp.where(
        (lax.broadcasted_iota(jnp.int32, (16, 128), 1) >= REST) & (lax.broadcasted_iota(jnp.int32, (16, 128), 1) < REST + 3), 1.0, 0.0
    ).astype(BF16)
    scale_out = lax.dot_general(
        picked, hidden_v[1].reshape(TOKENS, 256)[:, 128:256], (((1,), (1,)), ((), ())), preferred_element_type=F32
    )[0:1]
    block = branch_total(1, part)
    norm = over_features(block * block)
    norm_v[...] = norm

    def tell(k, carry):
        other = k + 1
        there_z, there_y = lax.rem(z + other // NY, NZ), lax.rem(y + other % NY, NY)
        push(norm_v, norms_v.at[r], 17, {"ra": there_z * NY + there_y})
        return carry

    lax.fori_loop(0, NR - 1, tell, 0)
    norms_v[r] = norm
    pending.append((norms_v.at[pl.ds(0, NR - 1)], send_sem.at[17]))
    stream1 = RESIDUAL * stream_v[y] + gained_v[y] * scale_out
    post = jnp.zeros((FEATURES, 1), F32)
    for q in range(NY):
        post = jnp.where(y == q, columns[:, 8 * q + 3 : 8 * q + 4], post)
    all_of(norms_v.at[pl.ds(0, NR - 1)], recv_sem.at[17])
    norm = norms_v[0]
    for k in range(1, NR):
        norm = norm + norms_v[k]
    scale_out = lax.rsqrt(norm / D + EPSILON)
    out_ref[...] = (RESIDUAL * stream1 + block * post * scale_out).astype(BF16)
    for ref, sem in pending:
        all_of(ref, sem)


def per_device(tokens, pre_gain, post_gain, gate_weight, up_weight, down_weight):
    out = pl.pallas_call(
        kernel,
        out_shape=jax.ShapeDtypeStruct((FEATURES, TOKENS), BF16),
        in_specs=[pl.BlockSpec(memory_space=pl.ANY)] * 6,
        out_specs=pl.BlockSpec(memory_space=pltpu.VMEM),
        scratch_shapes=[
            pltpu.VMEM((FEATURES, TOKENS), BF16),
            pltpu.VMEM((2, 2, FEATURES), F32),
            pltpu.VMEM((2, FEATURES, UNITS), BF16),
            pltpu.VMEM((2, FEATURES, UNITS), BF16),
            pltpu.VMEM((2, FEATURES, UNITS), BF16),
            pltpu.VMEM((NY, FEATURES, TOKENS), BF16),
            pltpu.VMEM((NY, 2, 2, FEATURES), F32),
            pltpu.VMEM((2, NY, FEATURES, 384), BF16),
            pltpu.VMEM((2, NY, FEATURES, 384), BF16),
            pltpu.VMEM((2, NY, FEATURES, 256), BF16),
            pltpu.VMEM((2, NY, FEATURES, 256), BF16),
            pltpu.VMEM((1, TOKENS), F32),
            pltpu.VMEM((NZ, 1, TOKENS), F32),
            pltpu.VMEM((3, NZ, ROWS, 384), BF16),
            pltpu.VMEM((3, NZ, ROWS, 384), BF16),
            pltpu.VMEM((2, ROWS, 256), BF16),
            pltpu.VMEM((2, NZ, ROWS, 256), BF16),
            pltpu.VMEM((2, NY, FEATURES, TOKENS), BF16),
            pltpu.VMEM((NY, FEATURES, TOKENS), F32),
            pltpu.VMEM((2, NY, FEATURES, TOKENS), BF16),
            pltpu.VMEM((2, FEATURES, TOKENS), BF16),
            pltpu.VMEM((2, NC, FEATURES, TOKENS), BF16),
            pltpu.VMEM((FEATURES, TOKENS), F32),
            pltpu.VMEM((NY, FEATURES, TOKENS), F32),
            pltpu.VMEM((NY, FEATURES, TOKENS), F32),
            pltpu.VMEM((NY, FEATURES, TOKENS), F32),
            pltpu.VMEM((1, TOKENS), F32),
            pltpu.VMEM((NR, 1, TOKENS), F32),
            pltpu.SemaphoreType.DMA((6,)),
            pltpu.SemaphoreType.DMA((18,)),
            pltpu.SemaphoreType.DMA((18,)),
        ],
        compiler_params=pltpu.CompilerParams(collective_id=0, has_side_effects=True),
    )(tokens.T, pre_gain, post_gain, gate_weight, up_weight, down_weight.swapaxes(1, 2))
    return out.T


def solution(mesh):
    return jax.shard_map(
        per_device,
        mesh=mesh,
        in_specs=(
            P(None, "ra"),
            P(None, "ra"),
            P(None, "ra"),
            P(None, "ra", "cb"),
            P(None, "ra", "cb"),
            P(None, "cb", "ra"),
        ),
        out_specs=P(None, "ra"),
        check_vma=False,
    )
```

```python
import jax
import jax.numpy as jnp
from jax import lax
from jax.experimental import pallas as pl
from jax.experimental.pallas import tpu as pltpu
from jax.sharding import PartitionSpec as P

MESH = pl.DeviceIdType.MESH
F32, BF16 = jnp.float32, jnp.bfloat16

D = 2048
EPSILON = 1e-06
RESIDUAL = 0.25
NY, NZ, NC = 4, 8, 8
NR = NY * NZ
TOKENS = 128
ROWS = TOKENS // NZ
FEATURES = D // NR
UNITS = 704
REST = 48
STAT = 96
Z_ORDER = (4, 3, 5, 2, 6, 1, 7)
Y_ORDER = (2, 1, 3)


def terms(value):
    high = value.astype(BF16).astype(F32)
    left = value - high
    middle = left.astype(BF16).astype(F32)
    return [high, middle, left - middle]


def joined(tile, lane):
    return tile[:, lane : lane + 1] + tile[:, lane + 1 : lane + 2] + tile[:, lane + 2 : lane + 3]


def silu(value):
    return value / (1.0 + jnp.exp(-value))


def over_features(value):
    return jnp.sum(value, axis=0, keepdims=True)


def all_of(ref, sem):
    pltpu.make_async_copy(ref, ref, sem).wait()


def kernel(
    tokens_hbm, pre_hbm, post_hbm, gate_hbm, up_hbm, down_hbm, out_ref,
    tokens_v, gains_v, gate_v, up_v, down_v, tokens4_v, gains4_v,
    wide_from_v, wide_v, tall_from_v, tall_v,
    sent_v, got_v, mine_v, hidden_v,
    piece_v, own_v, pieces_v, part_v, parts_v, block_v, branch_v, shared_v, shares_v, stream_v, gained_v, norm_v, norms_v,
    load_sem, send_sem, recv_sem,
):
    r, c = lax.axis_index("ra"), lax.axis_index("cb")
    z, y = r // NY, r % NY
    pending = []

    def to_z(dz):
        there = lax.rem(z + dz, NZ)
        return there, {"ra": there * NY + y}

    def to_y(dy):
        there = lax.rem(y + dy, NY)
        return there, {"ra": z * NY + there}

    def to_c(dc):
        there = lax.rem(c + dc, NC)
        return there, {"cb": there}

    def push(src, dst, which, device):
        pltpu.make_async_remote_copy(
            src_ref=src, dst_ref=dst, send_sem=send_sem.at[which], recv_sem=recv_sem.at[which],
            device_id=device, device_id_type=MESH,
        ).start()

    barrier = pltpu.get_barrier_semaphore()
    for device in [to_z(k)[1] for k in range(1, NZ)] + [to_y(k)[1] for k in range(1, NY)] + [to_c(k)[1] for k in range(1, NC)]:
        pl.semaphore_signal(barrier, inc=1, device_id=device, device_id_type=MESH)

    loads = [
        pltpu.make_async_copy(gate_hbm, gate_v, load_sem.at[0]),
        pltpu.make_async_copy(up_hbm, up_v, load_sem.at[1]),
        pltpu.make_async_copy(tokens_hbm, tokens_v, load_sem.at[2]),
        pltpu.make_async_copy(pre_hbm, gains_v.at[0], load_sem.at[3]),
        pltpu.make_async_copy(post_hbm, gains_v.at[1], load_sem.at[4]),
        pltpu.make_async_copy(down_hbm, down_v, load_sem.at[5]),
    ]
    for load in loads:
        load.start()

    lane64 = lax.broadcasted_iota(jnp.int32, (FEATURES, 128), 1)

    def tail(ref, l):
        return jnp.concatenate([ref[l, :, 512:704].astype(F32), jnp.zeros((FEATURES, 64), F32)], axis=1)

    def shifted(value, lanes):
        lanes = lanes % 256
        return pltpu.roll(value, lanes, 1)[:, 0:128] if lanes else value[:, 0:128]

    def arrange_wide(l):
        gate_tail, up_tail = tail(gate_v, l), tail(up_v, l)
        for q in range(NY):
            wide_from_v[l, q, :, 0:128] = gate_v[l, :, q * 128 : q * 128 + 128]
            wide_from_v[l, q, :, 128:256] = up_v[l, :, q * 128 : q * 128 + 128]
            rest = jnp.where(
                lane64 < REST, shifted(gate_tail, -REST * q), jnp.where(lane64 < 2 * REST, shifted(up_tail, REST - REST * q), 0.0)
            )
            wide_from_v[l, q, :, 256:384] = rest.astype(BF16)

    def arrange_tall(l):
        down_tail = tail(down_v, l)
        for q in range(NY):
            tall_from_v[l, q, :, 0:128] = down_v[l, :, q * 128 : q * 128 + 128]
            tall_from_v[l, q, :, 128:256] = jnp.where(lane64 < REST, shifted(down_tail, -REST * q), 0.0).astype(BF16)

    def exchange_wide(l):
        for dy in Y_ORDER:
            there, device = to_y(dy)
            push(wide_from_v.at[l, there], wide_v.at[l, y], l, device)
        wide_v[l, y] = wide_from_v[l, y]
        pending.append((wide_from_v.at[l, pl.ds(0, NY - 1)], send_sem.at[l]))

    def exchange_tall(l):
        for dy in Y_ORDER:
            there, device = to_y(dy)
            push(tall_from_v.at[l, there], tall_v.at[l, y], 2 + l, device)
        tall_v[l, y] = tall_from_v[l, y]
        pending.append((tall_from_v.at[l, pl.ds(0, NY - 1)], send_sem.at[2 + l]))

    loads[0].wait()
    loads[1].wait()
    arrange_wide(0)
    for load in loads[2:]:
        load.wait()
    pl.semaphore_wait(barrier, NZ - 1 + NY - 1 + NC - 1)


    for dy in Y_ORDER:
        push(tokens_v, tokens4_v.at[y], 4, to_y(dy)[1])
        push(gains_v, gains4_v.at[y], 5, to_y(dy)[1])
    tokens4_v[y] = tokens_v[...]
    gains4_v[y] = gains_v[...]
    pending.append((tokens4_v.at[pl.ds(0, NY - 1)], send_sem.at[4]))
    pending.append((gains4_v.at[pl.ds(0, NY - 1)], send_sem.at[5]))
    exchange_wide(0)

    arrange_tall(0)
    exchange_tall(0)
    all_of(tokens4_v.at[pl.ds(0, NY - 1)], recv_sem.at[4])
    stream0 = tokens4_v[...].reshape(NY * FEATURES, TOKENS).astype(F32)
    arrange_wide(1)
    exchange_wide(1)
    arrange_tall(1)
    exchange_tall(1)

    all_of(gains4_v.at[pl.ds(0, NY - 1)], recv_sem.at[5])
    lines = []
    for q in range(NY):
        lines += [gains4_v[q, 0], gains4_v[q, 1], jnp.zeros((4, FEATURES), F32)]
    lines = jnp.concatenate(lines + [jnp.zeros((128 - 8 * NY, FEATURES), F32)], axis=0)
    columns = jnp.concatenate([lines, jnp.zeros((128, 128 - FEATURES), F32)], axis=1).T[0:FEATURES]

    def gain(i):
        return jnp.concatenate([columns[:, 8 * q + i : 8 * q + i + 1] for q in range(NY)], axis=0)


    passing = jnp.where(
        lax.broadcasted_iota(jnp.int32, (128, 128), 0) == lax.broadcasted_iota(jnp.int32, (128, 128), 1) - STAT, 1.0, 0.0
    ).astype(BF16)

    def multiply(l, slot, features, statistics):
        left = features.T
        high = left.astype(BF16)
        wide = wide_v[l].reshape(NY * FEATURES, 384)
        low = (left - high.astype(F32)).astype(BF16)
        part = jnp.dot(high, wide, preferred_element_type=F32) + jnp.dot(low, wide, preferred_element_type=F32)
        last = part[:, 256:384]
        if statistics:
            lines = [t for s in statistics for t in terms(s)]
            lines = jnp.concatenate(lines + [jnp.zeros((128 - len(lines), 128), F32)], axis=0)
            last = last + jnp.dot(lines.T.astype(BF16), passing, preferred_element_type=F32)
        sent_v[slot, :, :, 0:256] = part[:, 0:256].reshape(NZ, ROWS, 256).astype(BF16)
        sent_v[slot, :, :, 256:384] = last.reshape(NZ, ROWS, 128).astype(BF16)

    def scatter(slot):
        for dz in Z_ORDER:
            there, device = to_z(dz)
            push(sent_v.at[slot, there], got_v.at[slot, dz], 7 + slot, device)
        pending.append((got_v.at[slot, pl.ds(1, NZ - 1)], send_sem.at[7 + slot]))

    def total(slot):
        all_of(got_v.at[slot, pl.ds(1, NZ - 1)], recv_sem.at[7 + slot])
        acc = sent_v[slot, z].astype(F32)
        for k in range(1, NZ):
            acc = acc + got_v[slot, k].astype(F32)
        return acc

    small_lane = lax.broadcasted_iota(jnp.int32, (ROWS, 128), 1)

    def broadcast_hidden(l, acc, extra):
        rest = acc[:, 256:384]
        main = silu(acc[:, 0:128]) * acc[:, 128:256]
        rest = jnp.where(small_lane < REST, silu(rest) * pltpu.roll(rest, 128 - REST, 1), 0.0)
        if extra is not None:
            for i, term in enumerate(terms(extra)):
                rest = jnp.where(small_lane == REST + i, term, rest)
        both = jnp.concatenate([main, rest], axis=1).astype(BF16)
        mine_v[l] = both
        for dz in Z_ORDER:
            push(mine_v.at[l], hidden_v.at[l, z], 10 + l, to_z(dz)[1])
        hidden_v[l, z] = both
        pending.append((hidden_v.at[l, pl.ds(0, NZ - 1)], send_sem.at[10 + l]))

    def project(l):
        all_of(tall_v.at[l, pl.ds(0, NY - 1)], recv_sem.at[2 + l])
        all_of(hidden_v.at[l, pl.ds(0, NZ - 1)], recv_sem.at[10 + l])
        right = hidden_v[l].reshape(TOKENS, 256)
        return lax.dot_general(
            tall_v[l].reshape(NY * FEATURES, 256), right, (((1,), (1,)), ((), ())), preferred_element_type=F32
        )

    def branch_total(l, part):
        part = part.reshape(NY, FEATURES, TOKENS)
        piece_v[l] = part.astype(BF16)
        for dy in Y_ORDER:
            there, device = to_y(dy)
            push(piece_v.at[l, there], pieces_v.at[l, dy], 12 + l, device)
        own_v[...] = part
        pending.append((pieces_v.at[l, pl.ds(1, NY - 1)], send_sem.at[12 + l]))
        all_of(pieces_v.at[l, pl.ds(1, NY - 1)], recv_sem.at[12 + l])
        acc = own_v[y]
        for k in range(1, NY):
            acc = acc + pieces_v[l, k].astype(F32)
        rounded = acc.astype(BF16)
        part_v[l] = rounded
        for dc in range(1, NC):
            push(part_v.at[l], parts_v.at[l, c], 14 + l, to_c(dc)[1])
        parts_v[l, c] = rounded
        pending.append((parts_v.at[l, pl.ds(0, NC - 1)], send_sem.at[14 + l]))
        all_of(parts_v.at[l, pl.ds(0, NC - 1)], recv_sem.at[14 + l])
        acc = parts_v[l, 0].astype(F32)
        for k in range(1, NC):
            acc = acc + parts_v[l, k].astype(F32)
        return acc

    xy = [(dy, dx, dk) for dy in (2, 1, 3, 0) for dx in (2, 1, 3, 0) for dk in (0, 1) if dy or dx or dk]

    def to_xy(step):
        dy, dx, dk = step
        there_y = lax.rem(y + dy, NY)
        there_c = lax.rem(c // 2 + dx, 4) * 2 + lax.rem(c % 2 + dk, 2)
        return there_y, there_c, {"ra": z * NY + there_y, "cb": there_c}

    def scatter_xy(part):
        shared_v[...] = part.reshape(NY, NC, 8, TOKENS)
        for k, step in enumerate(xy):
            there_y, there_c, device = to_xy(step)
            push(shared_v.at[there_y, there_c], shares_v.at[k], 12, device)
        pending.append((shares_v, send_sem.at[12]))

    def total_xy():
        all_of(shares_v, recv_sem.at[12])
        acc = shared_v[y, c]
        for k in range(len(xy)):
            acc = acc + shares_v[k]
        return acc

    def gather_xy(block):
        block_v[...] = block
        for step in xy:
            push(block_v, branch_v.at[y, c], 16, to_xy(step)[2])
        branch_v[y, c] = block
        pending.append((shares_v, send_sem.at[16]))
        all_of(shares_v, recv_sem.at[16])

    gains = [gain(i) for i in range(3)]
    all_of(wide_v.at[0, pl.ds(0, NY - 1)], recv_sem.at[0])
    multiply(0, 0, stream0 * gains[0], [over_features(stream0 * stream0)])
    scatter(0)
    acc = total(0)
    squares = joined(acc[:, 256:384], STAT)
    acc = acc * lax.rsqrt(squares / D + EPSILON)
    broadcast_hidden(0, acc, None)
    all_of(wide_v.at[1, pl.ds(0, NY - 1)], recv_sem.at[1])
    multiply(1, 1, stream0 * gains[1], [])
    scatter(1)
    part = project(0)
    scatter_xy(part)
    block = total_xy()
    gather_xy(block)
    branch = branch_v[...].reshape(NY * FEATURES, TOKENS)
    gained = branch * gains[2]

    multiply(1, 2, gained * gains[1], [over_features(branch * branch), over_features(gained * gained), over_features(stream0 * gained)])
    scatter(2)
    stream_v[...] = stream0.reshape(NY, FEATURES, TOKENS)
    gained_v[...] = gained.reshape(NY, FEATURES, TOKENS)
    early = total(1)
    acc = total(2)
    rest = acc[:, 256:384]
    scale_out = lax.rsqrt(joined(rest, STAT) / D + EPSILON)
    squares = (
        RESIDUAL * RESIDUAL * squares
        + 2.0 * RESIDUAL * scale_out * joined(rest, STAT + 6)
        + scale_out * scale_out * joined(rest, STAT + 3)
    )
    scale = lax.rsqrt(squares / D + EPSILON)
    acc = scale * (RESIDUAL * early + scale_out * acc)
    broadcast_hidden(1, acc, scale_out)
    part = project(1)
    picked = jnp.where(
        (lax.broadcasted_iota(jnp.int32, (16, 128), 1) >= REST) & (lax.broadcasted_iota(jnp.int32, (16, 128), 1) < REST + 3), 1.0, 0.0
    ).astype(BF16)
    scale_out = lax.dot_general(
        picked, hidden_v[1].reshape(TOKENS, 256)[:, 128:256], (((1,), (1,)), ((), ())), preferred_element_type=F32
    )[0:1]
    block = branch_total(1, part)
    norm = over_features(block * block)
    norm_v[...] = norm

    def tell(k, carry):
        other = k + 1
        there_z, there_y = lax.rem(z + other // NY, NZ), lax.rem(y + other % NY, NY)
        push(norm_v, norms_v.at[r], 17, {"ra": there_z * NY + there_y})
        return carry

    lax.fori_loop(0, NR - 1, tell, 0)
    norms_v[r] = norm
    pending.append((norms_v.at[pl.ds(0, NR - 1)], send_sem.at[17]))
    stream1 = RESIDUAL * stream_v[y] + gained_v[y] * scale_out
    post = jnp.zeros((FEATURES, 1), F32)
    for q in range(NY):
        post = jnp.where(y == q, columns[:, 8 * q + 3 : 8 * q + 4], post)
    all_of(norms_v.at[pl.ds(0, NR - 1)], recv_sem.at[17])
    norm = norms_v[0]
    for k in range(1, NR):
        norm = norm + norms_v[k]
    scale_out = lax.rsqrt(norm / D + EPSILON)
    out_ref[...] = (RESIDUAL * stream1 + block * post * scale_out).astype(BF16)
    for ref, sem in pending:
        all_of(ref, sem)


def per_device(tokens, pre_gain, post_gain, gate_weight, up_weight, down_weight):
    out = pl.pallas_call(
        kernel,
        out_shape=jax.ShapeDtypeStruct((FEATURES, TOKENS), BF16),
        in_specs=[pl.BlockSpec(memory_space=pl.ANY)] * 6,
        out_specs=pl.BlockSpec(memory_space=pltpu.VMEM),
        scratch_shapes=[
            pltpu.VMEM((FEATURES, TOKENS), BF16),
            pltpu.VMEM((2, 2, FEATURES), F32),
            pltpu.VMEM((2, FEATURES, UNITS), BF16),
            pltpu.VMEM((2, FEATURES, UNITS), BF16),
            pltpu.VMEM((2, FEATURES, UNITS), BF16),
            pltpu.VMEM((NY, FEATURES, TOKENS), BF16),
            pltpu.VMEM((NY, 2, 2, FEATURES), F32),
            pltpu.VMEM((2, NY, FEATURES, 384), BF16),
            pltpu.VMEM((2, NY, FEATURES, 384), BF16),
            pltpu.VMEM((2, NY, FEATURES, 256), BF16),
            pltpu.VMEM((2, NY, FEATURES, 256), BF16),
            pltpu.VMEM((3, NZ, ROWS, 384), BF16),
            pltpu.VMEM((3, NZ, ROWS, 384), BF16),
            pltpu.VMEM((2, ROWS, 256), BF16),
            pltpu.VMEM((2, NZ, ROWS, 256), BF16),
            pltpu.VMEM((2, NY, FEATURES, TOKENS), BF16),
            pltpu.VMEM((NY, FEATURES, TOKENS), F32),
            pltpu.VMEM((2, NY, FEATURES, TOKENS), BF16),
            pltpu.VMEM((2, FEATURES, TOKENS), BF16),
            pltpu.VMEM((2, NC, FEATURES, TOKENS), BF16),
            pltpu.VMEM((8, TOKENS), F32),
            pltpu.VMEM((NY, NC, 8, TOKENS), F32),
            pltpu.VMEM((NY, NC, 8, TOKENS), F32),
            pltpu.VMEM((NR - 1, 8, TOKENS), F32),
            pltpu.VMEM((NY, FEATURES, TOKENS), F32),
            pltpu.VMEM((NY, FEATURES, TOKENS), F32),
            pltpu.VMEM((1, TOKENS), F32),
            pltpu.VMEM((NR, 1, TOKENS), F32),
            pltpu.SemaphoreType.DMA((6,)),
            pltpu.SemaphoreType.DMA((18,)),
            pltpu.SemaphoreType.DMA((18,)),
        ],
        compiler_params=pltpu.CompilerParams(collective_id=0, has_side_effects=True),
    )(tokens.T, pre_gain, post_gain, gate_weight, up_weight, down_weight.swapaxes(1, 2))
    return out.T


def solution(mesh):
    return jax.shard_map(
        per_device,
        mesh=mesh,
        in_specs=(
            P(None, "ra"),
            P(None, "ra"),
            P(None, "ra"),
            P(None, "ra", "cb"),
            P(None, "ra", "cb"),
            P(None, "cb", "ra"),
        ),
        out_specs=P(None, "ra"),
        check_vma=False,
    )
```

```python
import jax
import jax.numpy as jnp
from jax import lax
from jax.experimental import pallas as pl
from jax.experimental.pallas import tpu as pltpu
from jax.sharding import PartitionSpec as P

MESH = pl.DeviceIdType.MESH
F32, BF16 = jnp.float32, jnp.bfloat16

D = 2048
EPSILON = 1e-06
RESIDUAL = 0.25
NY, NZ, NC = 4, 8, 8
NR = NY * NZ
TOKENS = 128
ROWS = TOKENS // NZ
FEATURES = D // NR
UNITS = 704
REST = 48
STAT = 96
Z_ORDER = (4, 3, 5, 2, 6, 1, 7)
Y_ORDER = (2, 1, 3)


def terms(value):
    high = value.astype(BF16).astype(F32)
    left = value - high
    middle = left.astype(BF16).astype(F32)
    return [high, middle, left - middle]


def joined(tile, lane):
    return tile[:, lane : lane + 1] + tile[:, lane + 1 : lane + 2] + tile[:, lane + 2 : lane + 3]


def silu(value):
    return value / (1.0 + jnp.exp(-value))


def over_features(value):
    return jnp.sum(value, axis=0, keepdims=True)


def all_of(ref, sem):
    pltpu.make_async_copy(ref, ref, sem).wait()


def kernel(
    tokens_hbm, pre_hbm, post_hbm, gate_hbm, up_hbm, down_hbm, out_ref,
    tokens_v, gains_v, gate_v, up_v, down_v, tokens4_v, gains4_v,
    wide_from_v, wide_v, tall_from_v, tall_v,
    sent_v, got_v, mine_v, hidden_v,
    piece_v, own_v, pieces_v, part_v, parts_v, block_v, branch_v, shared_v, shares_v, stream_v, gained_v, norm_v, norms_v,
    load_sem, send_sem, recv_sem, near_sem, far_sem,
):
    r, c = lax.axis_index("ra"), lax.axis_index("cb")
    z, y = r // NY, r % NY
    pending = []

    def to_z(dz):
        there = lax.rem(z + dz, NZ)
        return there, {"ra": there * NY + y}

    def to_y(dy):
        there = lax.rem(y + dy, NY)
        return there, {"ra": z * NY + there}

    def to_c(dc):
        there = lax.rem(c + dc, NC)
        return there, {"cb": there}

    def push(src, dst, which, device):
        pltpu.make_async_remote_copy(
            src_ref=src, dst_ref=dst, send_sem=send_sem.at[which], recv_sem=recv_sem.at[which],
            device_id=device, device_id_type=MESH,
        ).start()

    barrier = pltpu.get_barrier_semaphore()
    for device in [to_z(k)[1] for k in (1, NZ - 1)] + [to_y(k)[1] for k in range(1, NY)] + [to_c(k)[1] for k in range(1, NC)]:
        pl.semaphore_signal(barrier, inc=1, device_id=device, device_id_type=MESH)

    loads = [
        pltpu.make_async_copy(gate_hbm, gate_v, load_sem.at[0]),
        pltpu.make_async_copy(up_hbm, up_v, load_sem.at[1]),
        pltpu.make_async_copy(tokens_hbm, tokens_v, load_sem.at[2]),
        pltpu.make_async_copy(pre_hbm, gains_v.at[0], load_sem.at[3]),
        pltpu.make_async_copy(post_hbm, gains_v.at[1], load_sem.at[4]),
        pltpu.make_async_copy(down_hbm, down_v, load_sem.at[5]),
    ]
    for load in loads:
        load.start()

    lane64 = lax.broadcasted_iota(jnp.int32, (FEATURES, 128), 1)

    def tail(ref, l):
        return jnp.concatenate([ref[l, :, 512:704].astype(F32), jnp.zeros((FEATURES, 64), F32)], axis=1)

    def shifted(value, lanes):
        lanes = lanes % 256
        return pltpu.roll(value, lanes, 1)[:, 0:128] if lanes else value[:, 0:128]

    def arrange_wide(l):
        gate_tail, up_tail = tail(gate_v, l), tail(up_v, l)
        for q in range(NY):
            wide_from_v[l, q, :, 0:128] = gate_v[l, :, q * 128 : q * 128 + 128]
            wide_from_v[l, q, :, 128:256] = up_v[l, :, q * 128 : q * 128 + 128]
            rest = jnp.where(
                lane64 < REST, shifted(gate_tail, -REST * q), jnp.where(lane64 < 2 * REST, shifted(up_tail, REST - REST * q), 0.0)
            )
            wide_from_v[l, q, :, 256:384] = rest.astype(BF16)

    def arrange_tall(l):
        down_tail = tail(down_v, l)
        for q in range(NY):
            tall_from_v[l, q, :, 0:128] = down_v[l, :, q * 128 : q * 128 + 128]
            tall_from_v[l, q, :, 128:256] = jnp.where(lane64 < REST, shifted(down_tail, -REST * q), 0.0).astype(BF16)

    def exchange_wide(l):
        for dy in Y_ORDER:
            there, device = to_y(dy)
            push(wide_from_v.at[l, there], wide_v.at[l, y], l, device)
        wide_v[l, y] = wide_from_v[l, y]
        pending.append((wide_from_v.at[l, pl.ds(0, NY - 1)], send_sem.at[l]))

    def exchange_tall(l):
        for dy in Y_ORDER:
            there, device = to_y(dy)
            push(tall_from_v.at[l, there], tall_v.at[l, y], 2 + l, device)
        tall_v[l, y] = tall_from_v[l, y]
        pending.append((tall_from_v.at[l, pl.ds(0, NY - 1)], send_sem.at[2 + l]))

    loads[0].wait()
    loads[1].wait()
    arrange_wide(0)
    for load in loads[2:]:
        load.wait()
    pl.semaphore_wait(barrier, 2 + NY - 1 + NC - 1)


    for dy in Y_ORDER:
        push(tokens_v, tokens4_v.at[y], 4, to_y(dy)[1])
        push(gains_v, gains4_v.at[y], 5, to_y(dy)[1])
    tokens4_v[y] = tokens_v[...]
    gains4_v[y] = gains_v[...]
    pending.append((tokens4_v.at[pl.ds(0, NY - 1)], send_sem.at[4]))
    pending.append((gains4_v.at[pl.ds(0, NY - 1)], send_sem.at[5]))
    exchange_wide(0)
    for dz in (1, NZ - 1):
        pl.semaphore_signal(near_sem, inc=1, device_id=to_z(dz)[1], device_id_type=MESH)
    arrange_tall(0)
    pl.semaphore_wait(near_sem, 2)
    for dz in (2, NZ - 2):
        pl.semaphore_signal(far_sem, inc=1, device_id=to_z(dz)[1], device_id_type=MESH)
    arrange_wide(1)
    arrange_tall(1)
    all_of(tokens4_v.at[pl.ds(0, NY - 1)], recv_sem.at[4])
    stream0 = tokens4_v[...].reshape(NY * FEATURES, TOKENS).astype(F32)

    all_of(gains4_v.at[pl.ds(0, NY - 1)], recv_sem.at[5])
    lines = []
    for q in range(NY):
        lines += [gains4_v[q, 0], gains4_v[q, 1], jnp.zeros((4, FEATURES), F32)]
    lines = jnp.concatenate(lines + [jnp.zeros((128 - 8 * NY, FEATURES), F32)], axis=0)
    columns = jnp.concatenate([lines, jnp.zeros((128, 128 - FEATURES), F32)], axis=1).T[0:FEATURES]

    def gain(i):
        return jnp.concatenate([columns[:, 8 * q + i : 8 * q + i + 1] for q in range(NY)], axis=0)

    passing = jnp.where(
        lax.broadcasted_iota(jnp.int32, (128, 128), 0) == lax.broadcasted_iota(jnp.int32, (128, 128), 1) - STAT, 1.0, 0.0
    ).astype(BF16)

    def multiply(l, slot, features, statistics):
        left = features.T
        high = left.astype(BF16)
        wide = wide_v[l].reshape(NY * FEATURES, 384)
        low = (left - high.astype(F32)).astype(BF16)
        part = jnp.dot(high, wide, preferred_element_type=F32) + jnp.dot(low, wide, preferred_element_type=F32)
        last = part[:, 256:384]
        if statistics:
            lines = [t for s in statistics for t in terms(s)]
            lines = jnp.concatenate(lines + [jnp.zeros((128 - len(lines), 128), F32)], axis=0)
            last = last + jnp.dot(lines.T.astype(BF16), passing, preferred_element_type=F32)
        sent_v[slot, :, :, 0:256] = part[:, 0:256].reshape(NZ, ROWS, 256).astype(BF16)
        sent_v[slot, :, :, 256:384] = last.reshape(NZ, ROWS, 128).astype(BF16)

    def scatter(slot):
        for dz in Z_ORDER:
            there, device = to_z(dz)
            push(sent_v.at[slot, there], got_v.at[slot, dz], 7 + slot, device)
        pending.append((got_v.at[slot, pl.ds(1, NZ - 1)], send_sem.at[7 + slot]))

    def total(slot):
        all_of(got_v.at[slot, pl.ds(1, NZ - 1)], recv_sem.at[7 + slot])
        acc = sent_v[slot, z].astype(F32)
        for k in range(1, NZ):
            acc = acc + got_v[slot, k].astype(F32)
        return acc

    small_lane = lax.broadcasted_iota(jnp.int32, (ROWS, 128), 1)

    def broadcast_hidden(l, acc, extra):
        rest = acc[:, 256:384]
        main = silu(acc[:, 0:128]) * acc[:, 128:256]
        rest = jnp.where(small_lane < REST, silu(rest) * pltpu.roll(rest, 128 - REST, 1), 0.0)
        if extra is not None:
            for i, term in enumerate(terms(extra)):
                rest = jnp.where(small_lane == REST + i, term, rest)
        both = jnp.concatenate([main, rest], axis=1).astype(BF16)
        mine_v[l] = both
        for dz in Z_ORDER:
            push(mine_v.at[l], hidden_v.at[l, z], 10 + l, to_z(dz)[1])
        hidden_v[l, z] = both
        pending.append((hidden_v.at[l, pl.ds(0, NZ - 1)], send_sem.at[10 + l]))

    def project(l):
        all_of(tall_v.at[l, pl.ds(0, NY - 1)], recv_sem.at[2 + l])
        all_of(hidden_v.at[l, pl.ds(0, NZ - 1)], recv_sem.at[10 + l])
        right = hidden_v[l].reshape(TOKENS, 256)
        return lax.dot_general(
            tall_v[l].reshape(NY * FEATURES, 256), right, (((1,), (1,)), ((), ())), preferred_element_type=F32
        )

    def branch_total(l, part):
        part = part.reshape(NY, FEATURES, TOKENS)
        piece_v[l] = part.astype(BF16)
        for dy in Y_ORDER:
            there, device = to_y(dy)
            push(piece_v.at[l, there], pieces_v.at[l, dy], 12 + l, device)
        own_v[...] = part
        pending.append((pieces_v.at[l, pl.ds(1, NY - 1)], send_sem.at[12 + l]))
        all_of(pieces_v.at[l, pl.ds(1, NY - 1)], recv_sem.at[12 + l])
        acc = own_v[y]
        for k in range(1, NY):
            acc = acc + pieces_v[l, k].astype(F32)
        rounded = acc.astype(BF16)
        part_v[l] = rounded
        for dc in range(1, NC):
            push(part_v.at[l], parts_v.at[l, c], 14 + l, to_c(dc)[1])
        parts_v[l, c] = rounded
        pending.append((parts_v.at[l, pl.ds(0, NC - 1)], send_sem.at[14 + l]))
        all_of(parts_v.at[l, pl.ds(0, NC - 1)], recv_sem.at[14 + l])
        acc = parts_v[l, 0].astype(F32)
        for k in range(1, NC):
            acc = acc + parts_v[l, k].astype(F32)
        return acc

    xy = [(dy, dx, dk) for dy in (2, 1, 3, 0) for dx in (2, 1, 3, 0) for dk in (0, 1) if dy or dx or dk]

    def to_xy(step):
        dy, dx, dk = step
        there_y = lax.rem(y + dy, NY)
        there_c = lax.rem(c // 2 + dx, 4) * 2 + lax.rem(c % 2 + dk, 2)
        return there_y, there_c, {"ra": z * NY + there_y, "cb": there_c}

    def scatter_xy(part):
        shared_v[...] = part.reshape(NY, NC, 8, TOKENS)
        for k, step in enumerate(xy):
            there_y, there_c, device = to_xy(step)
            push(shared_v.at[there_y, there_c], shares_v.at[k], 12, device)
        pending.append((shares_v, send_sem.at[12]))

    def total_xy():
        all_of(shares_v, recv_sem.at[12])
        acc = shared_v[y, c]
        for k in range(len(xy)):
            acc = acc + shares_v[k]
        return acc

    def gather_xy(block):
        block_v[...] = block
        for step in xy:
            push(block_v, branch_v.at[y, c], 16, to_xy(step)[2])
        branch_v[y, c] = block
        pending.append((shares_v, send_sem.at[16]))
        all_of(shares_v, recv_sem.at[16])

    gains = [gain(i) for i in range(3)]
    all_of(wide_v.at[0, pl.ds(0, NY - 1)], recv_sem.at[0])
    multiply(0, 0, stream0 * gains[0], [over_features(stream0 * stream0)])
    pl.semaphore_wait(far_sem, 2)
    scatter(0)
    exchange_tall(0)
    exchange_wide(1)
    exchange_tall(1)
    acc = total(0)
    squares = joined(acc[:, 256:384], STAT)
    acc = acc * lax.rsqrt(squares / D + EPSILON)
    broadcast_hidden(0, acc, None)
    all_of(wide_v.at[1, pl.ds(0, NY - 1)], recv_sem.at[1])
    multiply(1, 1, stream0 * gains[1], [])
    scatter(1)
    part = project(0)
    scatter_xy(part)
    block = total_xy()
    gather_xy(block)
    branch = branch_v[...].reshape(NY * FEATURES, TOKENS)
    gained = branch * gains[2]

    multiply(1, 2, gained * gains[1], [over_features(branch * branch), over_features(gained * gained), over_features(stream0 * gained)])
    scatter(2)
    stream_v[...] = stream0.reshape(NY, FEATURES, TOKENS)
    gained_v[...] = gained.reshape(NY, FEATURES, TOKENS)
    early = total(1)
    acc = total(2)
    rest = acc[:, 256:384]
    scale_out = lax.rsqrt(joined(rest, STAT) / D + EPSILON)
    squares = (
        RESIDUAL * RESIDUAL * squares
        + 2.0 * RESIDUAL * scale_out * joined(rest, STAT + 6)
        + scale_out * scale_out * joined(rest, STAT + 3)
    )
    scale = lax.rsqrt(squares / D + EPSILON)
    acc = scale * (RESIDUAL * early + scale_out * acc)
    broadcast_hidden(1, acc, scale_out)
    part = project(1)
    picked = jnp.where(
        (lax.broadcasted_iota(jnp.int32, (16, 128), 1) >= REST) & (lax.broadcasted_iota(jnp.int32, (16, 128), 1) < REST + 3), 1.0, 0.0
    ).astype(BF16)
    scale_out = lax.dot_general(
        picked, hidden_v[1].reshape(TOKENS, 256)[:, 128:256], (((1,), (1,)), ((), ())), preferred_element_type=F32
    )[0:1]
    block = branch_total(1, part)
    norm = over_features(block * block)
    norm_v[...] = norm

    def tell(k, carry):
        other = k + 1
        there_z, there_y = lax.rem(z + other // NY, NZ), lax.rem(y + other % NY, NY)
        push(norm_v, norms_v.at[r], 17, {"ra": there_z * NY + there_y})
        return carry

    lax.fori_loop(0, NR - 1, tell, 0)
    norms_v[r] = norm
    pending.append((norms_v.at[pl.ds(0, NR - 1)], send_sem.at[17]))
    stream1 = RESIDUAL * stream_v[y] + gained_v[y] * scale_out
    post = jnp.zeros((FEATURES, 1), F32)
    for q in range(NY):
        post = jnp.where(y == q, columns[:, 8 * q + 3 : 8 * q + 4], post)
    all_of(norms_v.at[pl.ds(0, NR - 1)], recv_sem.at[17])
    norm = norms_v[0]
    for k in range(1, NR):
        norm = norm + norms_v[k]
    scale_out = lax.rsqrt(norm / D + EPSILON)
    out_ref[...] = (RESIDUAL * stream1 + block * post * scale_out).astype(BF16)
    for ref, sem in pending:
        all_of(ref, sem)


def per_device(tokens, pre_gain, post_gain, gate_weight, up_weight, down_weight):
    out = pl.pallas_call(
        kernel,
        out_shape=jax.ShapeDtypeStruct((FEATURES, TOKENS), BF16),
        in_specs=[pl.BlockSpec(memory_space=pl.ANY)] * 6,
        out_specs=pl.BlockSpec(memory_space=pltpu.VMEM),
        scratch_shapes=[
            pltpu.VMEM((FEATURES, TOKENS), BF16),
            pltpu.VMEM((2, 2, FEATURES), F32),
            pltpu.VMEM((2, FEATURES, UNITS), BF16),
            pltpu.VMEM((2, FEATURES, UNITS), BF16),
            pltpu.VMEM((2, FEATURES, UNITS), BF16),
            pltpu.VMEM((NY, FEATURES, TOKENS), BF16),
            pltpu.VMEM((NY, 2, 2, FEATURES), F32),
            pltpu.VMEM((2, NY, FEATURES, 384), BF16),
            pltpu.VMEM((2, NY, FEATURES, 384), BF16),
            pltpu.VMEM((2, NY, FEATURES, 256), BF16),
            pltpu.VMEM((2, NY, FEATURES, 256), BF16),
            pltpu.VMEM((3, NZ, ROWS, 384), BF16),
            pltpu.VMEM((3, NZ, ROWS, 384), BF16),
            pltpu.VMEM((2, ROWS, 256), BF16),
            pltpu.VMEM((2, NZ, ROWS, 256), BF16),
            pltpu.VMEM((2, NY, FEATURES, TOKENS), BF16),
            pltpu.VMEM((NY, FEATURES, TOKENS), F32),
            pltpu.VMEM((2, NY, FEATURES, TOKENS), BF16),
            pltpu.VMEM((2, FEATURES, TOKENS), BF16),
            pltpu.VMEM((2, NC, FEATURES, TOKENS), BF16),
            pltpu.VMEM((8, TOKENS), F32),
            pltpu.VMEM((NY, NC, 8, TOKENS), F32),
            pltpu.VMEM((NY, NC, 8, TOKENS), F32),
            pltpu.VMEM((NR - 1, 8, TOKENS), F32),
            pltpu.VMEM((NY, FEATURES, TOKENS), F32),
            pltpu.VMEM((NY, FEATURES, TOKENS), F32),
            pltpu.VMEM((1, TOKENS), F32),
            pltpu.VMEM((NR, 1, TOKENS), F32),
            pltpu.SemaphoreType.DMA((6,)),
            pltpu.SemaphoreType.DMA((18,)),
            pltpu.SemaphoreType.DMA((18,)),
            pltpu.SemaphoreType.REGULAR,
            pltpu.SemaphoreType.REGULAR,
        ],
        compiler_params=pltpu.CompilerParams(collective_id=0, has_side_effects=True),
    )(tokens.T, pre_gain, post_gain, gate_weight, up_weight, down_weight.swapaxes(1, 2))
    return out.T


def solution(mesh):
    return jax.shard_map(
        per_device,
        mesh=mesh,
        in_specs=(
            P(None, "ra"),
            P(None, "ra"),
            P(None, "ra"),
            P(None, "ra", "cb"),
            P(None, "ra", "cb"),
            P(None, "cb", "ra"),
        ),
        out_specs=P(None, "ra"),
        check_vma=False,
    )
```
